512 devices in a mesh: tp: 32 (over z, core), dp: 16 (over y, x).
Axes of the slice: x: 4, y: 4, z: 16, core: 2. Of those that a mesh axis runs over, the one named last changes fastest.
Arguments:
- tokens: bfloat16 [256, 4096], P(None, 'dp'), may hold values from -18 to 18
- lengths: int32 [256], P('dp'), may hold values from 1 to 16384, 540672 in all
- gain_one: float32 [4096], P('dp'), may hold values from 0.1 to 1.9
- recept_one: bfloat16 [4096, 2048], P('dp', 'tp'), may hold values from -0.09375 to 0.09375
- key_one: bfloat16 [4096, 2048], P('dp', 'tp'), may hold values from -0.09375 to 0.09375
- value_one: bfloat16 [4096, 2048], P('dp', 'tp'), may hold values from -0.09375 to 0.09375
- decay_one: bfloat16 [4096, 2048], P('dp', 'tp'), may hold values from -0.09375 to 0.09375
- learn_one: bfloat16 [4096, 2048], P('dp', 'tp'), may hold values from -0.09375 to 0.09375
- gate_one: bfloat16 [4096, 2048], P('dp', 'tp'), may hold values from -0.09375 to 0.09375
- pace_one: float32 [16, 2048], P(None, 'tp'), may hold values from -3 to 2
- group_one: float32 [2048], P('tp'), may hold values from 0.1 to 1.9
- output_one: bfloat16 [2048, 4096], P('tp', 'dp'), may hold values from -0.125 to 0.125
- state_one: float32 [256, 32, 4096], P('dp', 'tp'), may hold values from -3 to 3
- gain_two: float32 [4096], P('dp'), may hold values from 0.1 to 1.9
- recept_two: bfloat16 [4096, 2048], P('dp', 'tp'), may hold values from -0.09375 to 0.09375
- key_two: bfloat16 [4096, 2048], P('dp', 'tp'), may hold values from -0.09375 to 0.09375
- value_two: bfloat16 [4096, 2048], P('dp', 'tp'), may hold values from -0.09375 to 0.09375
- decay_two: bfloat16 [4096, 2048], P('dp', 'tp'), may hold values from -0.09375 to 0.09375
- learn_two: bfloat16 [4096, 2048], P('dp', 'tp'), may hold values from -0.09375 to 0.09375
- gate_two: bfloat16 [4096, 2048], P('dp', 'tp'), may hold values from -0.09375 to 0.09375
- pace_two: float32 [16, 2048], P(None, 'tp'), may hold values from -3 to 2
- group_two: float32 [2048], P('tp'), may hold values from 0.1 to 1.9
- output_two: bfloat16 [2048, 4096], P('tp', 'dp'), may hold values from -0.125 to 0.125
- state_two: float32 [256, 32, 4096], P('dp', 'tp'), may hold values from -3 to 3
Outputs:
- mixed: bfloat16 [256, 4096], P(None, 'dp')
- fresh_one: float32 [256, 32, 4096], P('dp', 'tp')
- fresh_two: float32 [256, 32, 4096], P('dp', 'tp')
The draws below stay inside these ranges and needn't reach their ends.
All inputs are finite; a program needn't handle non-finite values. No bound on the sum of `lengths` on one device may be relied on, other than what follows from the above.
Results may differ from the reference program's by a relative error of at most 0.0069.
Values may be sent and summed in bfloat16 or wider, within the bound.
No kernel may reach another device: no remote copies, remote signals or barrier semaphores. Data moves between devices by JAX's collectives and lax.ppermute only.
A program may use at most 64 MiB of HBM per device.

```python
import math
import jax
import jax.numpy as jnp
import numpy as np
from jax import lax

D = 4096
HEAD = 64
SPAN_LEN = 1024
MAX_LEN = 16384
SPANS = 16
HEADS = 32
WIDTH = 2048
BATCH = 256


def draw_tokens(key, part):
    first_key = jax.random.fold_in(key, 11)
    second_key = jax.random.fold_in(key, 12)
    groups = 16
    plain = jax.random.truncated_normal(first_key, -6.0, 6.0, (BATCH, D), jnp.float32)
    scales = jnp.exp(jax.random.uniform(second_key, (BATCH, groups, 1), jnp.float32, -1.0986, 1.0986))
    shaped = plain.reshape(BATCH, groups, D // groups) * scales
    return shaped.reshape(BATCH, D).astype(jnp.bfloat16)


def block_levels(stream_key, dims, split, least, top_value):
    gain, own = 1.0, jax.random.fold_in(stream_key, 6)
    for axis_at, parts in split:
        heights = jnp.exp(jax.random.uniform(jax.random.fold_in(own, axis_at), (parts,), jnp.float32, least / len(split), top_value / len(split)))
        gain = gain * jnp.repeat(heights, dims[axis_at] // parts).reshape([-1 if axis == axis_at else 1 for axis in range(len(dims))])
    return gain


def split_up(number_of, total, reach, slope):
    loads = [(1 << 20) // math.isqrt(rank ** slope) + 1 for rank in range(2, number_of + 1)]
    surplus, holding = total - reach - (number_of - 1), [1] * (number_of - 1)
    while surplus > 0:
        free = [i for i in range(number_of - 1) if holding[i] < reach]
        mass, remaining = sum([loads[i] for i in free]), surplus
        for i in free:
            extra = min(reach - holding[i], max(1, remaining * loads[i] // mass), surplus)
            holding[i] = holding[i] + extra
            surplus = surplus - extra
    return np.array([reach] + holding)


def ragged(rng, number_of, total, reach, lean):
    if number_of == 2:
        one = jax.random.randint(rng, (), max(1, total - reach), min(reach, total - 1) + 1)
        return jnp.stack([one, total - one])
    sizes = jnp.asarray(split_up(number_of, total, reach, lean), jnp.int32)
    pairs = (number_of - 1) // 2
    donor, receiver = sizes[1:1 + 2 * pairs:2], sizes[2:2 + 2 * pairs:2]
    slack = jnp.minimum(donor - 1, reach - receiver)
    shifted = jax.random.randint(jax.random.fold_in(rng, 1), (pairs,), 0, 1 << 20) % (slack + 1)
    sizes = sizes.at[1:1 + 2 * pairs:2].set(donor - shifted).at[2:2 + 2 * pairs:2].set(receiver + shifted)
    return sizes[jax.random.permutation(jax.random.fold_in(rng, 2), number_of)]


def bell_draw(own_key, extent, width, limit, split=(), held_as=jnp.bfloat16):
    drawn = jax.random.normal(own_key, extent, jnp.float32) * width
    if len(split) > 0:
        drawn = block_levels(own_key, extent, split, -0.22, 0.18) * drawn
    return jnp.clip(drawn, min=-limit, max=limit).astype(held_as)


def setup_inputs(seed: int = 0) -> dict:
    arg_keys = jax.random.split(jax.random.key(seed), 25)
    tokens = draw_tokens(jax.random.fold_in(arg_keys[24], 71), 0)
    lengths = ragged(arg_keys[1], BATCH, BATCH * 2048 + MAX_LEN, MAX_LEN, 2).astype(jnp.int32)
    gain_one = jnp.clip(1.0 + 0.18 * jax.random.normal(arg_keys[2], (D,), jnp.float32), 0.1, 1.9)
    recept_one = bell_draw(arg_keys[3], (D, WIDTH), D ** -0.5, 0.09375, ((0, 16), (1, 32)))
    key_one = bell_draw(arg_keys[4], (D, WIDTH), D ** -0.5, 0.09375, ((0, 16), (1, 32)))
    value_one = bell_draw(arg_keys[5], (D, WIDTH), D ** -0.5, 0.09375, ((0, 16), (1, 32)))
    decay_one = bell_draw(arg_keys[6], (D, WIDTH), D ** -0.5, 0.09375, ((0, 16), (1, 32)))
    learn_one = bell_draw(arg_keys[7], (D, WIDTH), D ** -0.5, 0.09375, ((0, 16), (1, 32)))
    gate_one = bell_draw(arg_keys[8], (D, WIDTH), D ** -0.5, 0.09375, ((0, 16), (1, 32)))
    pace_one = jnp.clip(-3.0 + 5.0 * jax.random.uniform(arg_keys[9], (SPANS, WIDTH), jnp.float32) ** block_levels(arg_keys[9], (SPANS, WIDTH), ((1, 32),), -0.2, 0.2), -3.0, 2.0)
    group_one = jnp.clip(1.0 + 0.18 * jax.random.normal(arg_keys[10], (WIDTH,), jnp.float32), 0.1, 1.9)
    output_one = bell_draw(arg_keys[11], (WIDTH, D), WIDTH ** -0.5, 0.125, ((0, 32), (1, 16)))
    state_one = bell_draw(arg_keys[12], (BATCH, HEADS, HEAD * HEAD), 0.5, 3.0, ((0, 16), (1, 32)), jnp.float32)
    gain_two = jnp.clip(1.0 + 0.18 * jax.random.normal(arg_keys[13], (D,), jnp.float32), 0.1, 1.9)
    recept_two = bell_draw(arg_keys[14], (D, WIDTH), D ** -0.5, 0.09375, ((0, 16), (1, 32)))
    key_two = bell_draw(arg_keys[15], (D, WIDTH), D ** -0.5, 0.09375, ((0, 16), (1, 32)))
    value_two = bell_draw(arg_keys[16], (D, WIDTH), D ** -0.5, 0.09375, ((0, 16), (1, 32)))
    decay_two = bell_draw(arg_keys[17], (D, WIDTH), D ** -0.5, 0.09375, ((0, 16), (1, 32)))
    learn_two = bell_draw(arg_keys[18], (D, WIDTH), D ** -0.5, 0.09375, ((0, 16), (1, 32)))
    gate_two = bell_draw(arg_keys[19], (D, WIDTH), D ** -0.5, 0.09375, ((0, 16), (1, 32)))
    pace_two = jnp.clip(-3.0 + 5.0 * jax.random.uniform(arg_keys[20], (SPANS, WIDTH), jnp.float32) ** block_levels(arg_keys[20], (SPANS, WIDTH), ((1, 32),), -0.2, 0.2), -3.0, 2.0)
    group_two = jnp.clip(1.0 + 0.18 * jax.random.normal(arg_keys[21], (WIDTH,), jnp.float32), 0.1, 1.9)
    output_two = bell_draw(arg_keys[22], (WIDTH, D), WIDTH ** -0.5, 0.125, ((0, 32), (1, 16)))
    state_two = bell_draw(arg_keys[23], (BATCH, HEADS, HEAD * HEAD), 0.5, 3.0, ((0, 16), (1, 32)), jnp.float32)
    return {"tokens": tokens, "lengths": lengths, "gain_one": gain_one, "recept_one": recept_one, "key_one": key_one, "value_one": value_one, "decay_one": decay_one, "learn_one": learn_one, "gate_one": gate_one, "pace_one": pace_one, "group_one": group_one, "output_one": output_one, "state_one": state_one, "gain_two": gain_two, "recept_two": recept_two, "key_two": key_two, "value_two": value_two, "decay_two": decay_two, "learn_two": learn_two, "gate_two": gate_two, "pace_two": pace_two, "group_two": group_two, "output_two": output_two, "state_two": state_two}


norm_eps = 1e-06
group_eps = 0.00064

def recur_block(hidden_in, lengths, norm_gain, recept, key_weight, value_weight, decay_weight, learn_weight, gate_weight, pace_table, group_gain, output_weight, old_state):
    floats = hidden_in.astype(jnp.float32)
    inverse = lax.rsqrt(lax.optimization_barrier(jnp.mean(floats * floats, axis=1, keepdims=True)) + norm_eps)
    scaled = (floats * norm_gain).astype(jnp.bfloat16)

    def project(weight):
        return inverse * jnp.dot(scaled, weight, preferred_element_type=jnp.float32)
    recept_rows = project(recept)
    key_rows = project(key_weight)
    value_rows = project(value_weight)
    span_index = ((lengths - 1) // SPAN_LEN).astype(jnp.int32)
    decay_in = project(decay_weight) + pace_table[span_index]
    decay_rate = jnp.exp(-jnp.exp(-jax.nn.softplus(-decay_in) - 0.5))
    learn_rate = jax.nn.sigmoid(project(learn_weight))
    gate_rows = jax.nn.sigmoid(project(gate_weight))
    batch_rows = hidden_in.shape[0]

    def split_heads(flat_field):
        return flat_field.reshape(batch_rows, HEADS, HEAD)
    recept_rows = split_heads(recept_rows)
    key_rows = split_heads(key_rows)
    value_rows = split_heads(value_rows)
    decay_rate = split_heads(decay_rate)
    learn_rate = split_heads(learn_rate)
    unit_key = key_rows * lax.rsqrt(lax.optimization_barrier(jnp.sum(key_rows * key_rows, axis=-1, keepdims=True)) + 1.0)
    matrix = old_state.reshape(batch_rows, HEADS, HEAD, HEAD)
    removed = jnp.einsum('bhvk,bhk->bhv', matrix, unit_key, precision=lax.Precision.HIGHEST)
    matrix = matrix * decay_rate[:, :, None, :] - removed[..., None] * (unit_key * learn_rate)[:, :, None, :] + value_rows[..., None] * (key_rows * learn_rate)[:, :, None, :]
    readout = jnp.einsum('bhvk,bhk->bhv', matrix, recept_rows, precision=lax.Precision.HIGHEST)
    center = readout - lax.optimization_barrier(jnp.mean(readout, axis=-1, keepdims=True))
    normed = center * lax.rsqrt(lax.optimization_barrier(jnp.mean(center * center, axis=-1, keepdims=True)) + group_eps)
    head_mix = (normed.reshape(batch_rows, HEADS * HEAD) * group_gain * gate_rows).astype(jnp.bfloat16)
    update = jnp.dot(head_mix, output_weight, preferred_element_type=jnp.float32)
    result = (floats + update).astype(jnp.bfloat16)
    return (result, matrix.reshape(batch_rows, HEADS, HEAD * HEAD))

def reference(tokens, lengths, gain_one, recept_one, key_one, value_one, decay_one, learn_one, gate_one, pace_one, group_one, output_one, state_one, gain_two, recept_two, key_two, value_two, decay_two, learn_two, gate_two, pace_two, group_two, output_two, state_two):
    middle, fresh_one = recur_block(tokens, lengths, gain_one, recept_one, key_one, value_one, decay_one, learn_one, gate_one, pace_one, group_one, output_one, state_one)
    mixed, fresh_two = recur_block(middle, lengths, gain_two, recept_two, key_two, value_two, decay_two, learn_two, gate_two, pace_two, group_two, output_two, state_two)
    return (mixed, fresh_one, fresh_two)
```

```python
import functools

import jax
import jax.numpy as jnp
from jax import lax
from jax.experimental import pallas as pl
from jax.experimental.pallas import tpu as pltpu
from jax.sharding import PartitionSpec as P

D = 4096
HEAD = 64
SPAN_SHIFT = 10
LANES = 128
norm_eps = 1e-06
group_eps = 0.00064
half_decay = 0.6065306597126334

f32 = jnp.float32
bf16 = jnp.bfloat16


def exchange(parts, axis):
    return lax.all_to_all(parts, axis, split_axis=0, concat_axis=0, tiled=True)


def dot_last(left, right):
    return lax.dot_general(left, right, (((1,), (1,)), ((), ())), preferred_element_type=f32)


def exact_dot(left, right):
    return jnp.dot(left, right, precision=lax.Precision.HIGHEST, preferred_element_type=f32)


def twice(rows):
    return jnp.concatenate([rows, rows], axis=1)


def sigmoid(values):
    return 1.0 / (1.0 + jnp.exp(-values))


def state_step(first, second, third, inverse, lengths, pace_ref, group, state):
    seqs = first.shape[0]
    tiles = state.shape[0] // seqs
    first, second, third = first * inverse, second * inverse, third * inverse
    recept, key = first[:, :HEAD], first[:, HEAD:]
    value, decay_in = second[:, :HEAD], second[:, HEAD:]
    learn_in, gate_in = third[:, :HEAD], third[:, HEAD:]
    span = (lengths - 1) >> SPAN_SHIFT
    for s in range(pace_ref.shape[0]):
        decay_in = decay_in + jnp.where(span == s, pace_ref[s : s + 1, :], 0.0)
    decay_rate = jnp.exp(-half_decay * sigmoid(decay_in))
    learn_rate = sigmoid(learn_in)
    gate_rows = sigmoid(gate_in)
    unit_key = key * lax.rsqrt(jnp.sum(key * key, axis=1, keepdims=True) + 1.0)

    lane = lax.broadcasted_iota(jnp.int32, (LANES, LANES), 0) // HEAD
    column = lax.broadcasted_iota(jnp.int32, (LANES, LANES), 1) // HEAD
    same_half = (lane == column).astype(f32)
    lane = lax.broadcasted_iota(jnp.int32, (LANES, HEAD), 0) // HEAD
    column = lax.broadcasted_iota(jnp.int32, (LANES, HEAD), 1) & 1
    to_values = (lane == column).astype(f32)
    lane = lax.broadcasted_iota(jnp.int32, (HEAD, LANES), 0) & 1
    column = lax.broadcasted_iota(jnp.int32, (HEAD, LANES), 1) // HEAD
    from_values = (lane == column).astype(f32)
    tile = lax.broadcasted_iota(jnp.int32, (seqs, tiles, HEAD), 1)
    own_tile = tile == (lax.broadcasted_iota(jnp.int32, (seqs, tiles, HEAD), 2) >> 1)

    def flat(cube):
        return cube.reshape(seqs * tiles, cube.shape[2])

    def cubed(rows):
        return rows.reshape(seqs, tiles, rows.shape[1])

    matrix = cubed(state)
    removed = cubed(exact_dot(flat(matrix * twice(unit_key)[:, None, :]), same_half))
    spread = jnp.where(own_tile, jnp.broadcast_to(value[:, None, :], own_tile.shape), 0.0)
    values = cubed(exact_dot(flat(spread), from_values))
    fresh = (
        matrix * twice(decay_rate)[:, None, :]
        - removed * twice(unit_key * learn_rate)[:, None, :]
        + values * twice(key * learn_rate)[:, None, :]
    )
    read = cubed(exact_dot(flat(fresh * twice(recept)[:, None, :]), to_values))
    readout = jnp.sum(jnp.where(own_tile, read, 0.0), axis=1)
    center = readout - jnp.mean(readout, axis=1, keepdims=True)
    normed = center * lax.rsqrt(jnp.mean(center * center, axis=1, keepdims=True) + group_eps)
    head_mix = (normed * group * gate_rows).astype(bf16)
    return head_mix, flat(fresh)


def pack_kernel(*refs):
    weights, output, gain, packed = refs[:6], refs[6], refs[7], refs[8]
    for i, weight in enumerate(weights):
        packed[HEAD * i : HEAD * (i + 1), :] = weight[...]
    packed[6 * HEAD : 7 * HEAD, :] = output[...]
    values = gain[...]
    high = values.astype(bf16).astype(f32)
    middle = (values - high).astype(bf16).astype(f32)
    low = values - high - middle
    row = lax.broadcasted_iota(jnp.int32, (16, values.shape[1]), 0)
    parts = jnp.where(row == 0, high, jnp.where(row == 1, middle, jnp.where(row == 2, low, 0.0)))
    packed[7 * HEAD :, :] = parts.astype(bf16)


def project_kernel(*refs):
    tokens, gain, weights, output, parts = refs[0], refs[1], refs[2:8], refs[8], refs[9]
    groups = parts.shape[0]
    rows = tokens.shape[0] // groups
    scaled = (tokens[...].astype(f32) * gain[...]).astype(bf16)
    for i in range(3):
        pair = jnp.concatenate([weights[2 * i][...], weights[2 * i + 1][...]], axis=0)
        product = dot_last(scaled, pair).astype(bf16)
        parts[:, rows * i : rows * (i + 1), :] = product.reshape(groups, rows, LANES)
    for h in range(2):
        columns = slice(LANES * h, LANES * (h + 1))
        start = rows * (3 + h)
        parts[:, start : start + rows, :] = tokens[:, columns].reshape(groups, rows, LANES)
        start = 5 * rows + HEAD * h
        parts[:, start : start + HEAD, :] = jnp.broadcast_to(
            output[:, columns][None], (groups, HEAD, LANES)
        )


def first_step_kernel(arrived, lengths, pace, group, state, parts, fresh):
    groups = arrived.shape[0]
    rows = parts.shape[1]
    sums = [
        jnp.sum(arrived[:, rows * i : rows * (i + 1), :].astype(f32), axis=0) for i in range(3)
    ]
    token_rows = arrived[:, 3 * rows : 4 * rows, :].astype(f32)
    other_rows = arrived[:, 4 * rows : 5 * rows, :].astype(f32)
    squares = jnp.sum(token_rows * token_rows + other_rows * other_rows, axis=0)
    squares = jnp.sum(squares, axis=1, keepdims=True)
    inverse = lax.rsqrt(squares / D + norm_eps)
    head_mix, new_state = state_step(
        *sums, inverse, lengths[...], pace, group[...], state[...]
    )
    for d in range(groups):
        for h in range(2):
            start = 5 * rows + HEAD * h
            product = jnp.dot(
                head_mix, arrived[d, start : start + HEAD, :], preferred_element_type=f32
            )
            parts[2 * d + h] = product.astype(bf16)
    fresh[...] = new_state


def second_step_kernel(
    middle, gathered, lengths, pace, group, state, parts, fresh, held, arrivals
):
    groups = held.shape[0]
    copies = [
        pltpu.make_async_copy(gathered.at[d], held.at[d], arrivals.at[d]) for d in range(groups)
    ]
    for copy in copies:
        copy.start()
    floats = middle[...].astype(f32)
    squares = jnp.sum(jnp.sum(floats * floats, axis=0), axis=1, keepdims=True)
    inverse = lax.rsqrt(squares / D + norm_eps)
    sums = jnp.zeros((floats.shape[1], 6 * HEAD), f32)
    for d in range(groups):
        copies[d].wait()
        gains = held[d, 7 * HEAD :, :].astype(f32)
        gain = gains[0:1] + gains[1:2] + gains[2:3]
        columns = jnp.concatenate([floats[2 * d], floats[2 * d + 1]], axis=1)
        scaled = (columns * gain).astype(bf16)
        sums = sums + dot_last(scaled, held[d, : 6 * HEAD, :])
    head_mix, new_state = state_step(
        sums[:, :LANES],
        sums[:, LANES : 2 * LANES],
        sums[:, 2 * LANES :],
        inverse,
        lengths[...],
        pace,
        group[...],
        state[...],
    )
    for d in range(groups):
        product = jnp.dot(
            head_mix, held[d, 6 * HEAD : 7 * HEAD, :], preferred_element_type=f32
        ).astype(bf16)
        parts[2 * d] = product[:, :LANES]
        parts[2 * d + 1] = product[:, LANES:]
    fresh[...] = new_state


def add_kernel(shares, own, copies, result):
    total = own[...].astype(f32) + jnp.sum(shares[...].astype(f32), axis=0)
    rounded = total.astype(bf16)
    result[...] = rounded
    copies[...] = jnp.broadcast_to(rounded[None], copies.shape)


def call(kernel, name, out_shape, *args, **options):
    return pl.pallas_call(kernel, name=name, out_shape=out_shape, **options)(*args)


def shape(*lengths, dtype=bf16):
    return jax.ShapeDtypeStruct(lengths, dtype)


def body(
    tokens,
    lengths,
    gain_one,
    recept_one,
    key_one,
    value_one,
    decay_one,
    learn_one,
    gate_one,
    pace_one,
    group_one,
    output_one,
    state_one,
    gain_two,
    recept_two,
    key_two,
    value_two,
    decay_two,
    learn_two,
    gate_two,
    pace_two,
    group_two,
    output_two,
    state_two,
):
    dp, tp = lax.axis_size("dp"), lax.axis_size("tp")
    rows, cols = tokens.shape
    seqs = rows // dp
    state_rows = seqs * HEAD * HEAD // LANES
    weights_one = [w.T for w in (recept_one, key_one, value_one, decay_one, learn_one, gate_one)]
    weights_two = [w.T for w in (recept_two, key_two, value_two, decay_two, learn_two, gate_two)]
    depth = 7 * HEAD + 16
    packed = call(
        pack_kernel, "pack", shape(depth, cols), *weights_two, output_two, gain_two[None]
    )
    gathered = lax.all_gather(packed, "dp")
    lengths = lengths[:, None]

    parts = call(
        project_kernel,
        "project",
        shape(dp, 5 * seqs + 2 * HEAD, LANES),
        tokens,
        gain_one[None],
        *weights_one,
        output_one,
    )
    arrived = exchange(parts, "dp")
    parts, fresh_one = call(
        first_step_kernel,
        "first_step",
        (shape(tp, seqs, LANES), shape(state_rows, LANES, dtype=f32)),
        arrived,
        lengths,
        pace_one,
        group_one[None],
        state_one.reshape(state_rows, LANES),
    )
    own = lax.axis_index("tp")
    own_tokens = lax.dynamic_slice(
        arrived, (own // 2, seqs * (3 + own % 2), 0), (1, seqs, LANES)
    )[0]
    both = (shape(tp, seqs, LANES), shape(seqs, LANES))
    copies, middle_own = call(add_kernel, "add_one", both, exchange(parts, "tp"), own_tokens)
    middle = exchange(copies, "tp")

    whole = functools.partial(pl.BlockSpec, memory_space=pltpu.VMEM)
    parts, fresh_two = call(
        second_step_kernel,
        "second_step",
        (shape(tp, seqs, LANES), shape(state_rows, LANES, dtype=f32)),
        middle,
        gathered,
        lengths,
        pace_two,
        group_two[None],
        state_two.reshape(state_rows, LANES),
        in_specs=[whole(), pl.BlockSpec(memory_space=pl.ANY), whole(), whole(), whole(), whole()],
        scratch_shapes=[pltpu.VMEM((dp, depth, cols), bf16), pltpu.SemaphoreType.DMA((dp,))],
    )
    copies, _ = call(add_kernel, "add_two", both, exchange(parts, "tp"), middle_own)
    mixed = exchange(exchange(copies, "tp"), "dp")
    mixed = mixed.reshape(dp, 2, seqs, LANES).transpose(0, 2, 1, 3).reshape(rows, cols)
    return mixed, fresh_one.reshape(seqs, 1, -1), fresh_two.reshape(seqs, 1, -1)


def solution(mesh):
    weight_specs = (P("dp", "tp"),) * 6
    block_specs = (
        P("dp"),
        *weight_specs,
        P(None, "tp"),
        P("tp"),
        P("tp", "dp"),
        P("dp", "tp", None),
    )
    in_specs = (P(None, "dp"), P("dp"), *block_specs, *block_specs)
    out_specs = (P(None, "dp"), P("dp", "tp", None), P("dp", "tp", None))
    return jax.shard_map(body, mesh=mesh, in_specs=in_specs, out_specs=out_specs, check_vma=False)
```
